32 devices in a mesh: grp: 2 (over x), ep: 16 (over z, y, core).
Axes of the slice: x: 2, y: 2, z: 4, core: 2. Of those that a mesh axis runs over, the one named last changes fastest.
Arguments:
- queries: bfloat16 [32, 8, 128], P(('grp', 'ep')), parts along dimension 0, may hold values from -400 to 400
- fresh_token_key: bfloat16 [32, 2, 128], P(('grp', 'ep')), parts along dimension 0, may hold values from -6 to 6
- value_new: bfloat16 [32, 2, 128], P(('grp', 'ep')), parts along dimension 0, may hold values from -6 to 6
- forget_logit: float32 [32, 8], P(('grp', 'ep')), parts along dimension 0, may hold values from -8 to 8
- cache_keys: bfloat16 [32, 2, 4096, 128], P(('grp', 'ep')), parts along dimension 0, may hold values from -12 to 12
- cache_values: bfloat16 [32, 2, 4096, 128], P(('grp', 'ep')), parts along dimension 0, may hold values from -6 to 6
- cache_cumlog: float32 [32, 8, 4096], P(('grp', 'ep')), parts along dimension 0, may hold values from -572 to 0
- lengths: int32 [32], P(('grp', 'ep')), parts along dimension 0, may hold values from 1024 to 4096
- residual: bfloat16 [32, 2048], P('grp', 'ep'), parts along dimension 0, may hold values from -6 to 6
- out_weight: bfloat16 [1024, 2048], P(None, 'ep'), may hold values from -0.1875 to 0.1875
- norm_gain: float32 [2048], replicated, may hold values from 0.1 to 1.9
- expert_gate: bfloat16 [16, 704, 2048], P('ep'), may hold values from -0.125 to 0.125
- expert_up: bfloat16 [16, 704, 2048], P('ep'), may hold values from -0.125 to 0.125
- expert_down: bfloat16 [16, 704, 2048], P('ep'), may hold values from -0.21875 to 0.21875
- shared_gate: bfloat16 [1408, 2048], P('ep'), may hold values from -0.125 to 0.125
- shared_up: bfloat16 [1408, 2048], P('ep'), may hold values from -0.125 to 0.125
- shared_down: bfloat16 [1408, 2048], P(None, 'ep'), may hold values from -0.15625 to 0.15625
- routes: int32 [32, 6], P('grp'), parts along dimension 0, may hold values from 0 to 15, all different within a row; in each aligned block of 16 rows (0 to 15, 16 to 31, ...) at most 12 rows name the same one
- route_scores: float32 [32, 6], P('grp'), parts along dimension 0, may hold values from 0.05 to 1
Outputs:
- updated: bfloat16 [32, 2048], P('grp', 'ep'), parts along dimension 0
The draws below stay inside these ranges and needn't reach their ends.
There are 2 independent parts, one for each index of `grp`. The reference program is written for one: setup_inputs(seed, part) draws one part's arguments, and reference() takes and returns one part's arrays. A program takes and returns all parts, laid end to end along the dimension named above; an argument that names none is the same for every part. Nothing has to cross between parts.
Inputs may be any that keep to these rules, and one draw needn't show every extreme that they name: `routes`: each row names 6 different experts; no expert is named by more than 12 rows of a part, a bound that some block reaches.
All inputs are finite; a program needn't handle non-finite values.
Results may differ from the reference program's by a relative error of at most 0.0068.
Values may be sent and summed in bfloat16 or wider, within the bound.
A program may use at most 64 MiB of HBM per device.

```python
import math
import jax
import jax.numpy as jnp
import numpy as np
from jax import lax

D = 2048
QUERY_HEADS = 8
HD = 128
KVH = 2
FF = 704
SHARED_FF = 1408
TOP_K = 6
CACHE_POSITIONS = 4096
SEQUENCE_TOTAL = 16
EXPERTS = 16
CAP = 12
QW = 1024


def draw_queries(key, part):
    sampled = jnp.clip(jax.random.normal(jax.random.fold_in(key, 511), (SEQUENCE_TOTAL, QUERY_HEADS, HD), jnp.float32), -6.0, 6.0)
    return sampled.astype(jnp.bfloat16)


def draw_cache_keys(key, part):
    sampled = jnp.clip(jax.random.normal(jax.random.fold_in(key, 521), (SEQUENCE_TOTAL, KVH, CACHE_POSITIONS, HD), jnp.float32), -6.0, 6.0)
    return sampled.astype(jnp.bfloat16)


def draw_cache_cumlog(key, part):
    slow_share = 0.5
    slow_heads = jax.random.uniform(jax.random.fold_in(key, 531), (SEQUENCE_TOTAL, QUERY_HEADS), jnp.float32) < slow_share
    seq_factor = 2.0 ** jax.random.uniform(jax.random.fold_in(key, 532), (SEQUENCE_TOTAL, 1, 1), jnp.float32, -1.0, 1.0)
    decay_rate = jnp.where(slow_heads, 1.0 / CACHE_POSITIONS, 1.0 / 40.0)[:, :, None] * seq_factor
    jitter_strength = jax.random.uniform(jax.random.fold_in(key, 533), (SEQUENCE_TOTAL, QUERY_HEADS, CACHE_POSITIONS), jnp.float32, 0.2, 1.8)
    cluster_positions = jax.random.uniform(jax.random.fold_in(key, 534), (SEQUENCE_TOTAL, 1, CACHE_POSITIONS), jnp.float32) < 4.0 / CACHE_POSITIONS
    cluster_length = jnp.log(jax.random.uniform(jax.random.fold_in(key, 535), (SEQUENCE_TOTAL, QUERY_HEADS, CACHE_POSITIONS), jnp.float32, 0.5, 0.8))
    step_log_gate = -decay_rate * jitter_strength + jnp.where(cluster_positions, cluster_length, 0.0)
    return jnp.cumsum(step_log_gate, axis=2)


def set_ends(result, stream_key, smallest, high):
    extent = result.shape
    index_at = [jax.random.randint(jax.random.fold_in(stream_key, axis), (), 0, extent[axis]) for axis in range(len(extent))]
    result = result.at[tuple(index_at)].set(smallest)
    longest = extent.index(max(extent))
    index_at[longest] = (index_at[longest] + 1) % extent[longest]
    return result.at[tuple(index_at)].set(high)


def block_scale(rng, shape, split, smallest, high):
    def one(dim, parts):
        steps = jax.random.uniform(jax.random.fold_in(jax.random.fold_in(rng, 6), dim), (parts,), jnp.float32, smallest / len(split), high / len(split))
        return jnp.repeat(jnp.exp(steps), shape[dim] // parts).reshape((-1,) + (1,) * (len(shape) - dim - 1))

    loudness = one(*split[0])
    for cut in split[1:]:
        loudness = loudness * one(*cut)
    return loudness


def deal_out(key, own, number, rows, amount, top, bound, skew):
    sequence = jax.random.permutation(key, amount)
    crowded, usual = shares(amount, rows * top, bound, skew, True), shares(amount, rows * top, bound, skew, False)
    places = jnp.arange(amount)

    def named(tallies, turn):
        used = int((tallies > 0).sum())
        fixed = max(1, used // 4)
        passed = fixed + (places - fixed + turn * (used - fixed)) % max(1, amount - fixed)
        return jnp.zeros((amount,), jnp.int32).at[sequence[jnp.where(places < fixed, places, passed)]].set(jnp.asarray(tallies, jnp.int32))

    tallies = jnp.where(number % 4 == 0, named(crowded, number // 4), named(usual, number - number // 4 - 1))
    mixed = jax.random.permutation(jax.random.fold_in(own, 3), amount)
    source_of, receiver = mixed[0:amount // 2 * 2:2], mixed[1:amount // 2 * 2:2]
    slack = jnp.minimum(tallies[source_of] - 1, bound - tallies[receiver]) // 2
    slack = jnp.where((source_of == sequence[0]) | (receiver == sequence[0]) | (tallies[receiver] == 0), 0, jnp.maximum(slack, 0))
    passed = jax.random.randint(jax.random.fold_in(own, 4), (amount // 2,), 0, 1 << 20) % (slack + 1)
    tallies = tallies.at[source_of].add(-passed).at[receiver].add(passed)
    labels = jnp.searchsorted(jnp.cumsum(tallies), jnp.arange(rows * top), side="right").astype(jnp.int32)
    table = labels.reshape(top, rows).T
    table = table[jax.random.permutation(jax.random.fold_in(own, 1), rows)]
    turn = jax.random.randint(jax.random.fold_in(own, 2), (rows, 1), 0, top)
    return jnp.take_along_axis(table, (jnp.arange(top)[None, :] + turn) % top, axis=1)


def shares(number_of, total, reach, skew, full):
    weights = [(1 << 20) // math.isqrt(grade ** skew) + 1 for grade in range(1, number_of + 1)]
    largest = reach if full else min(reach, max(-(-total // number_of), total * weights[0] // sum(weights)))
    least = 1 if total - largest >= number_of - 1 else 0
    counts, surplus = [largest] + [least] * (number_of - 1), total - largest - least * (number_of - 1)
    while surplus > 0:
        movable = [i for i in range(1, number_of) if counts[i] < largest] or [i for i in range(1, number_of) if counts[i] < reach]
        mass, remaining = sum([weights[i] for i in movable]), surplus
        for i in movable:
            more = min(reach - counts[i], max(1, remaining * weights[i] // mass), surplus)
            counts[i] = counts[i] + more
            surplus = surplus - more
    return np.array(counts)


def gaussian(rng, dims, width, most, split=(), held_as=jnp.bfloat16):
    array = jax.random.normal(rng, dims, jnp.float32) * width
    if len(split) > 0:
        array = block_scale(rng, dims, split, -0.22, 0.18) * array
    return jnp.clip(array, min=-most, max=most).astype(held_as)


def setup_inputs(seed: int = 0, part: int = 0) -> dict:
    splits = jax.random.split(jax.random.key(seed), 20)
    own_keys = jax.random.split(jax.random.fold_in(splits[19], part), 20)
    queries = draw_queries(jax.random.fold_in(jax.random.fold_in(splits[19], part), 71), part)
    fresh_token_key = gaussian(own_keys[1], (SEQUENCE_TOTAL, KVH, HD), 1.0, 6.0, ((0, 16),))
    value_new = gaussian(own_keys[2], (SEQUENCE_TOTAL, KVH, HD), 1.0, 6.0, ((0, 16),))
    forget_logit = gaussian(own_keys[3], (SEQUENCE_TOTAL, QUERY_HEADS), 2.0, 8.0, ((0, 16),), jnp.float32)
    cache_keys = draw_cache_keys(jax.random.fold_in(jax.random.fold_in(splits[19], part), 71), part)
    cache_values = gaussian(own_keys[5], (SEQUENCE_TOTAL, KVH, CACHE_POSITIONS, HD), 1.0, 6.0, ((0, 16),))
    cache_cumlog = draw_cache_cumlog(jax.random.fold_in(jax.random.fold_in(splits[19], part), 71), part)
    lengths = set_ends(jax.random.randint(own_keys[7], (SEQUENCE_TOTAL,), CACHE_POSITIONS // 4, CACHE_POSITIONS + 1), jax.random.fold_in(own_keys[7], 1), CACHE_POSITIONS // 4, CACHE_POSITIONS).astype(jnp.int32)
    residual = gaussian(own_keys[8], (SEQUENCE_TOTAL, D), 1.0, 6.0, ((1, 16),))
    out_weight = gaussian(splits[9], (QW, D), QW ** -0.5, 0.1875, ((1, 16),))
    norm_gain = jnp.clip(1.0 + 0.18 * jax.random.normal(splits[10], (D,), jnp.float32), 0.1, 1.9)
    expert_gate = gaussian(splits[11], (EXPERTS, FF, D), D ** -0.5, 0.125, ((0, 16),))
    expert_up = gaussian(splits[12], (EXPERTS, FF, D), D ** -0.5, 0.125, ((0, 16),))
    expert_down = gaussian(splits[13], (EXPERTS, FF, D), FF ** -0.5, 0.21875, ((0, 16),))
    shared_gate = gaussian(splits[14], (SHARED_FF, D), D ** -0.5, 0.125, ((0, 16),))
    shared_up = gaussian(splits[15], (SHARED_FF, D), D ** -0.5, 0.125, ((0, 16),))
    shared_down = gaussian(splits[16], (SHARED_FF, D), SHARED_FF ** -0.5, 0.15625, ((1, 16),))
    routes_keys = jax.random.split(jax.random.fold_in(own_keys[17], 1), SEQUENCE_TOTAL // SEQUENCE_TOTAL)
    routes_turns = jax.random.permutation(jax.random.fold_in(own_keys[17], 3), SEQUENCE_TOTAL // SEQUENCE_TOTAL)
    routes = jax.vmap(lambda own, number: deal_out(jax.random.fold_in(own_keys[17], 2), own, number, SEQUENCE_TOTAL, EXPERTS, TOP_K, CAP, 2))(routes_keys, routes_turns).reshape((SEQUENCE_TOTAL, TOP_K))
    route_scores = jnp.clip(jax.random.uniform(own_keys[18], (SEQUENCE_TOTAL, TOP_K), jnp.float32, 0.05, 1.0), 0.05, 1.0)
    return dict(queries=queries, fresh_token_key=fresh_token_key, value_new=value_new, forget_logit=forget_logit, cache_keys=cache_keys, cache_values=cache_values, cache_cumlog=cache_cumlog, lengths=lengths, residual=residual, out_weight=out_weight, norm_gain=norm_gain, expert_gate=expert_gate, expert_up=expert_up, expert_down=expert_down, shared_gate=shared_gate, shared_up=shared_up, shared_down=shared_down, routes=routes, route_scores=route_scores)


norm_eps = 1e-06
routed_scale = 2.5
contract_last = (((1,), (1,)), ((), ()))

def expert_hidden(row_block, gate_matrix, up_matrix):
    gate_part = lax.dot_general(row_block, gate_matrix, contract_last, preferred_element_type=jnp.float32)
    up_part = lax.dot_general(row_block, up_matrix, contract_last, preferred_element_type=jnp.float32)
    return (jax.nn.silu(gate_part) * up_part).astype(jnp.bfloat16)

def attend_one(packed):
    queries, fresh_token_key, value_new, forget_logit, cache_keys, cache_values, cache_cumlog, length = packed
    head_count, head_size = queries.shape
    key_heads, cache_span, _ = cache_keys.shape
    groups = head_count // key_heads
    inv_root = head_size ** (-0.5)
    grouped_heads = queries.astype(jnp.float32).reshape(key_heads, groups, head_size)
    scores = jnp.einsum('kgd,kpd->kgp', grouped_heads, cache_keys.astype(jnp.float32)).reshape(head_count, cache_span) * inv_root
    positions = jnp.arange(cache_span, dtype=jnp.int32)[None, :]
    latest = lax.optimization_barrier(jnp.sum(jnp.where(positions == length - 1, cache_cumlog, jnp.zeros_like(cache_cumlog)), axis=1))
    log_gate = jax.nn.log_sigmoid(forget_logit)
    scores = scores + (latest + log_gate)[:, None] - cache_cumlog
    visible = positions < length
    scores = jnp.where(visible, scores, -jnp.inf)
    own_score = jnp.einsum('kgd,kd->kg', grouped_heads, fresh_token_key.astype(jnp.float32)).reshape(head_count) * inv_root
    top_score = jnp.maximum(lax.optimization_barrier(jnp.max(scores, axis=1)), own_score)
    weights = jnp.where(visible, jnp.exp(scores - top_score[:, None]), jnp.zeros_like(scores))
    own_weight = jnp.exp(own_score - top_score)
    denominator = lax.optimization_barrier(jnp.sum(weights, axis=1)) + own_weight
    rounded = lax.optimization_barrier(weights.astype(jnp.bfloat16)).astype(jnp.float32)
    own_rounded = lax.optimization_barrier(own_weight.astype(jnp.bfloat16)).astype(jnp.float32)
    weighted = jnp.einsum('kgp,kpd->kgd', rounded.reshape(key_heads, groups, cache_span), cache_values.astype(jnp.float32)).reshape(head_count, head_size)
    own_value = jnp.repeat(value_new.astype(jnp.float32), groups, axis=0)
    numerator = weighted + own_rounded[:, None] * own_value
    return (numerator / denominator[:, None]).astype(jnp.bfloat16).reshape(head_count * head_size)

def reference(queries, fresh_token_key, value_new, forget_logit, cache_keys, cache_values, cache_cumlog, lengths, residual, out_weight, norm_gain, expert_gate, expert_up, expert_down, shared_gate, shared_up, shared_down, routes, route_scores):
    attended = lax.map(attend_one, (queries, fresh_token_key, value_new, forget_logit, cache_keys, cache_values, cache_cumlog, lengths))
    mixed = jnp.dot(attended, out_weight, preferred_element_type=jnp.float32)
    stream = (residual.astype(jnp.float32) + mixed).astype(jnp.bfloat16)
    rows_wide = stream.astype(jnp.float32)
    inv_rms = lax.rsqrt(lax.optimization_barrier(jnp.mean(rows_wide * rows_wide, axis=1, keepdims=True)) + norm_eps)
    normed = (rows_wide * inv_rms * norm_gain).astype(jnp.bfloat16)
    gate_weights = route_scores / lax.optimization_barrier(jnp.sum(route_scores, axis=1, keepdims=True)) * routed_scale
    slot_ids = jnp.arange(CAP, dtype=jnp.int32)[:, None]

    def one_expert(totals, packed):
        expert_id, gate_matrix, up_matrix, down_matrix = packed
        expert_hits = routes == expert_id
        is_member = lax.optimization_barrier(jnp.sum(expert_hits.astype(jnp.int32), axis=1)).astype(jnp.int32)
        token_share = lax.optimization_barrier(jnp.sum(jnp.where(expert_hits, gate_weights, jnp.zeros_like(gate_weights)), axis=1))
        slot_rank = (jnp.cumsum(is_member) - 1).astype(jnp.int32)
        selector = (is_member[None, :] == 1) & (slot_rank[None, :] == slot_ids)
        picked = jnp.dot(selector.astype(jnp.bfloat16), normed, preferred_element_type=jnp.float32).astype(jnp.bfloat16)
        hidden = expert_hidden(picked, gate_matrix, up_matrix)
        expert_out = jnp.dot(hidden, down_matrix, preferred_element_type=jnp.float32).astype(jnp.bfloat16)
        slot_share = jnp.dot(selector.astype(jnp.float32), token_share, precision=lax.Precision.HIGHEST)
        contribution = jnp.dot(selector.astype(jnp.float32).T, expert_out.astype(jnp.float32) * slot_share[:, None], precision=lax.Precision.HIGHEST)
        return (totals + contribution, None)
    routed, _ = lax.scan(one_expert, jnp.zeros(stream.shape, jnp.float32), (jnp.arange(EXPERTS, dtype=jnp.int32), expert_gate, expert_up, expert_down))
    shared_mid = expert_hidden(normed, shared_gate, shared_up)
    shared = jnp.dot(shared_mid, shared_down, preferred_element_type=jnp.float32)
    return (stream.astype(jnp.float32) + routed + shared).astype(jnp.bfloat16)
```

```python
import functools

import jax
import jax.numpy as jnp
from jax import lax
from jax.experimental import pallas as pl
from jax.experimental.pallas import tpu as pltpu
from jax.sharding import PartitionSpec as P

norm_eps = 1e-06
routed_scale = 2.5
contract_last = (((1,), (1,)), ((), ()))
LANES = 128
f32 = jnp.float32
bf16 = jnp.bfloat16


def dot_t(a, b):
    return lax.dot_general(a, b, contract_last, preferred_element_type=f32)


def join_lanes(blocks, width):
    if width % LANES == 0:
        return jnp.concatenate([b.astype(bf16) for b in blocks], axis=1)
    rows = blocks[0].shape[0]
    total = len(blocks) * width
    lane = lax.broadcasted_iota(jnp.int32, (rows, LANES), 1)
    pieces = [jnp.zeros((rows, LANES), f32) for _ in range(-(-total // LANES))]
    for k, block in enumerate(blocks):
        at, shift = divmod(k * width, LANES)
        moved = jnp.where(lane < width, block.astype(f32), 0.0)
        if shift:
            moved = pltpu.roll(moved, shift, 1)
        if shift + width <= LANES:
            pieces[at] = pieces[at] + moved
        else:
            pieces[at] = pieces[at] + jnp.where(lane >= shift, moved, 0.0)
            pieces[at + 1] = pieces[at + 1] + jnp.where(lane < shift, moved, 0.0)
    return jnp.concatenate([p.astype(bf16) for p in pieces], axis=1)[:, :total]


def widen(block):
    rows, width = block.shape
    short = -width % LANES
    if not short:
        return block
    return jnp.concatenate([block, jnp.zeros((rows, short), block.dtype)], axis=1)


def layer(
    n,
    lengths_ref,
    q_ref,
    fresh_ref,
    vnew_ref,
    forget_ref,
    residual_ref,
    gain_ref,
    routes_ref,
    route_scores_ref,
    keys_hbm,
    values_hbm,
    cumlog_hbm,
    out_w_hbm,
    gate_hbm,
    up_hbm,
    down_hbm,
    sgate_hbm,
    sup_hbm,
    sdown_hbm,
    out_ref,
    keys,
    values,
    cumlog,
    out_w,
    gate_w,
    up_w,
    down_w,
    sgate_w,
    sup_w,
    sdown_w,
    scores,
    att_buf,
    att_wide,
    stream_buf,
    mid_buf,
    eo_src,
    eo_buf,
    load_sem,
    key_sem,
    value_sem,
    send_sem,
    recv_sem,
):
    me = lax.axis_index("ep")
    heads, head_size = q_ref.shape[1:]
    key_heads, span = keys.shape[:2]
    groups = heads // key_heads
    rows, width = residual_ref.shape
    model = gate_w.shape[1]
    shared_width = sgate_w.shape[0]
    chunks = key_sem.shape[0]
    chunk = span // chunks

    def key_copy(c):
        part = pl.ds(c * chunk, chunk)
        return pltpu.make_async_copy(keys_hbm.at[0, :, part], keys.at[:, part], key_sem.at[c])

    def value_copy(c):
        part = pl.ds(c * chunk, chunk)
        return pltpu.make_async_copy(values_hbm.at[0, :, part], values.at[:, part], value_sem.at[c])

    cumlog_copy = pltpu.make_async_copy(cumlog_hbm.at[0], cumlog, load_sem.at[0])
    out_w_copy = pltpu.make_async_copy(out_w_hbm, out_w, load_sem.at[1])
    sgate_copy = pltpu.make_async_copy(sgate_hbm, sgate_w, load_sem.at[2])
    sup_copy = pltpu.make_async_copy(sup_hbm, sup_w, load_sem.at[3])
    gate_copy = pltpu.make_async_copy(gate_hbm.at[0], gate_w, load_sem.at[4])
    up_copy = pltpu.make_async_copy(up_hbm.at[0], up_w, load_sem.at[5])
    down_copy = pltpu.make_async_copy(down_hbm.at[0], down_w, load_sem.at[6])
    sdown_copy = pltpu.make_async_copy(sdown_hbm, sdown_w, load_sem.at[7])

    cumlog_copy.start()
    for c in range(chunks):
        key_copy(c).start()
    for c in range(chunks):
        value_copy(c).start()
    out_w_copy.start()

    barrier = pltpu.get_barrier_semaphore()

    def greet(i, carry):
        pl.semaphore_signal(barrier, inc=1, device_id={"ep": lax.rem(me + i, n)})
        return carry

    lax.fori_loop(1, n, greet, 0)

    def remote(phase, src, dst, peer, slot):
        return pltpu.make_async_remote_copy(
            src_ref=src,
            dst_ref=dst,
            send_sem=send_sem.at[phase, peer],
            recv_sem=recv_sem.at[phase, slot],
            device_id={"ep": peer},
        )

    def spread(phase, buf):
        def one(i, carry):
            peer = lax.rem(me + i, n)
            remote(phase, buf.at[me], buf.at[me], peer, me).start()
            return carry

        lax.fori_loop(1, n, one, 0)

    def arrive(phase, buf):
        def one(i, carry):
            peer = lax.rem(me + i, n)
            remote(phase, buf.at[peer], buf.at[peer], peer, peer).wait_recv()
            return carry

        lax.fori_loop(1, n, one, 0)

    def sent(phase, buf):
        def one(i, carry):
            peer = lax.rem(me + i, n)
            remote(phase, buf.at[peer], buf.at[peer], peer, peer).wait_send()
            return carry

        lax.fori_loop(1, n, one, 0)

    inv_root = head_size ** (-0.5)
    length = lengths_ref[0]
    q = q_ref[0]
    head_row = lax.broadcasted_iota(jnp.int32, (heads, head_size), 0)
    q_wide = jnp.concatenate(
        [jnp.where(head_row // groups == k, q, jnp.zeros_like(q)) for k in range(key_heads)], axis=1
    )
    fresh, vnew = fresh_ref[0].astype(f32), vnew_ref[0].astype(f32)
    own_key, own_value = fresh[0:1], vnew[0:1]
    for k in range(1, key_heads):
        own_key = jnp.where(head_row // groups == k, fresh[k : k + 1], own_key)
        own_value = jnp.where(head_row // groups == k, vnew[k : k + 1], own_value)
    own_score = jnp.sum(q.astype(f32) * own_key, axis=1, keepdims=True) * inv_root
    eye = lax.broadcasted_iota(jnp.int32, (heads, heads), 0) == lax.broadcasted_iota(
        jnp.int32, (heads, heads), 1
    )
    forget = jnp.sum(jnp.where(eye, forget_ref[...], 0.0), axis=1, keepdims=True)
    log_gate = jnp.minimum(forget, 0.0) - jnp.log1p(jnp.exp(-jnp.abs(forget)))

    cumlog_copy.wait()
    position = lax.broadcasted_iota(jnp.int32, (heads, span), 1)
    latest = (
        jnp.sum(jnp.where(position == length - 1, cumlog[...], 0.0), axis=1, keepdims=True)
        + log_gate
    )
    place = lax.broadcasted_iota(jnp.int32, (heads, chunk), 1)
    top = own_score
    for c in range(chunks):
        key_copy(c).wait()
        part = slice(c * chunk, (c + 1) * chunk)
        both = jnp.concatenate([keys[k, part] for k in range(key_heads)], axis=1)
        score = dot_t(q_wide, both) * inv_root + latest - cumlog[:, part]
        score = jnp.where(place + c * chunk < length, score, -jnp.inf)
        scores[:, part] = score
        top = jnp.maximum(top, jnp.max(score, axis=1, keepdims=True))

    sgate_copy.start()
    sup_copy.start()
    gate_copy.start()
    up_copy.start()
    down_copy.start()
    sdown_copy.start()

    own_weight = jnp.exp(own_score - top)
    denominator = own_weight
    weighted = jnp.zeros((heads, key_heads * head_size), f32)
    for c in range(chunks):
        value_copy(c).wait()
        part = slice(c * chunk, (c + 1) * chunk)
        weight = jnp.exp(scores[:, part] - top)
        denominator = denominator + jnp.sum(weight, axis=1, keepdims=True)
        both = jnp.concatenate([values[k, part] for k in range(key_heads)], axis=1)
        weighted = weighted + jnp.dot(weight.astype(bf16), both, preferred_element_type=f32)
    mine = weighted[:, :head_size]
    for k in range(1, key_heads):
        mine = jnp.where(
            head_row // groups == k, weighted[:, k * head_size : (k + 1) * head_size], mine
        )
    numerator = mine + own_weight.astype(bf16).astype(f32) * own_value
    att_buf[me] = (numerator / denominator).astype(bf16)

    pl.semaphore_wait(barrier, n - 1)
    spread(0, att_buf)

    route_scores = route_scores_ref[...]
    gate_weights = (
        route_scores / jnp.sum(route_scores, axis=1, keepdims=True) * routed_scale
    )
    expert_lane = lax.broadcasted_iota(jnp.int32, (rows, n), 1)
    share = jnp.zeros((rows, n), f32)
    for k in range(routes_ref.shape[1]):
        share = share + jnp.where(
            routes_ref[:, k : k + 1] == expert_lane, gate_weights[:, k : k + 1], 0.0
        )
    out_w_copy.wait()

    arrive(0, att_buf)
    att_wide[...] = att_buf[...].astype(f32).reshape(n * heads, head_size)
    attended = jnp.concatenate(
        [att_wide[pl.ds(h, n, stride=heads), :].astype(bf16) for h in range(heads)], axis=1
    )
    mixed = jnp.dot(attended, out_w[...], preferred_element_type=f32)
    stream = (residual_ref[...].astype(f32) + mixed).astype(bf16)
    stream_buf[me] = widen(stream)
    spread(1, stream_buf)
    sgate_copy.wait()
    sup_copy.wait()
    gate_copy.wait()
    up_copy.wait()
    arrive(1, stream_buf)

    full = join_lanes([stream_buf[j] for j in range(n)], width).astype(f32)
    inv_rms = lax.rsqrt(jnp.mean(full * full, axis=1, keepdims=True) + norm_eps)
    normed = (full * inv_rms * gain_ref[...]).astype(bf16)

    def hidden_of(gate, up):
        gated = dot_t(normed, gate)
        return (jax.nn.silu(gated) * dot_t(normed, up)).astype(bf16)

    mid_buf[me] = widen(hidden_of(sgate_w[...], sup_w[...]))
    spread(2, mid_buf)

    hidden = hidden_of(gate_w[...], up_w[...])
    down_copy.wait()
    wide = max(width, 2 * LANES)
    per = wide // width
    turns = model // wide

    def send_block(peer):
        remote(3, eo_src.at[peer], eo_buf.at[me], peer, me).start()

    for i in range(turns):
        c = lax.rem(me // per + 1 + i, turns)
        part = pl.ds(pl.multiple_of(c * wide, wide), wide)
        out = jnp.dot(hidden, down_w[:, part], preferred_element_type=f32).astype(bf16)
        for s in range(per):
            peer = c * per + s
            eo_src[peer] = widen(out[:, s * width : (s + 1) * width])
        for s in range(per):
            peer = c * per + s
            if i < turns - 1:
                send_block(peer)
            else:
                pl.when(peer != me)(functools.partial(send_block, peer))
    eo_buf[me] = eo_src[me]

    sdown_copy.wait()
    arrive(2, mid_buf)
    mid = join_lanes([mid_buf[j] for j in range(n)], shared_width)
    total = stream.astype(f32) + jnp.dot(mid, sdown_w[...], preferred_element_type=f32)
    arrive(3, eo_buf)
    for e in range(n):
        total = total + share[:, e : e + 1] * eo_buf[e][:, :width].astype(f32)
    out_ref[...] = total.astype(bf16)

    sent(0, att_buf)
    sent(1, stream_buf)
    sent(2, mid_buf)
    sent(3, eo_buf)


def solution(mesh):
    n = mesh.shape["ep"]

    def on_device(
        queries,
        fresh_token_key,
        value_new,
        forget_logit,
        cache_keys,
        cache_values,
        cache_cumlog,
        lengths,
        residual,
        out_weight,
        norm_gain,
        expert_gate,
        expert_up,
        expert_down,
        shared_gate,
        shared_up,
        shared_down,
        routes,
        route_scores,
    ):
        rows, width = residual.shape
        heads, head_size = queries.shape[1:]
        span = cache_keys.shape[2]
        lanes = -(-width // LANES) * LANES
        mid_lanes = -(-shared_gate.shape[0] // LANES) * LANES
        chunks = 4
        vmem = pl.BlockSpec(memory_space=pltpu.VMEM)
        hbm = pl.BlockSpec(memory_space=pl.ANY)

        def like(a, drop=0):
            return pltpu.VMEM(a.shape[drop:], a.dtype)

        return pl.pallas_call(
            functools.partial(layer, n),
            out_shape=jax.ShapeDtypeStruct((rows, width), bf16),
            in_specs=[pl.BlockSpec(memory_space=pltpu.SMEM)] + [vmem] * 8 + [hbm] * 10,
            out_specs=vmem,
            scratch_shapes=[
                like(cache_keys, 1),
                like(cache_values, 1),
                like(cache_cumlog, 1),
                like(out_weight),
                like(expert_gate, 1),
                like(expert_up, 1),
                like(expert_down, 1),
                like(shared_gate),
                like(shared_up),
                like(shared_down),
                pltpu.VMEM((heads, span), f32),
                pltpu.VMEM((n, heads, head_size), bf16),
                pltpu.VMEM((n * heads, head_size), f32),
                pltpu.VMEM((n, rows, lanes), bf16),
                pltpu.VMEM((n, rows, mid_lanes), bf16),
                pltpu.VMEM((n, rows, lanes), bf16),
                pltpu.VMEM((n, rows, lanes), bf16),
                pltpu.SemaphoreType.DMA((8,)),
                pltpu.SemaphoreType.DMA((chunks,)),
                pltpu.SemaphoreType.DMA((chunks,)),
                pltpu.SemaphoreType.DMA((4, n)),
                pltpu.SemaphoreType.DMA((4, n)),
            ],
            compiler_params=pltpu.CompilerParams(
                collective_id=0, has_side_effects=True, vmem_limit_bytes=48 * 1024 * 1024
            ),
            name="layer",
        )(
            lengths,
            queries,
            fresh_token_key,
            value_new,
            forget_logit,
            residual,
            norm_gain.reshape(1, -1),
            routes,
            route_scores,
            cache_keys,
            cache_values,
            cache_cumlog,
            out_weight,
            expert_gate,
            expert_up,
            expert_down,
            shared_gate,
            shared_up,
            shared_down,
        )

    placed = (
        P(("grp", "ep"), None, None),
        P(("grp", "ep"), None, None),
        P(("grp", "ep"), None, None),
        P(("grp", "ep"), None),
        P(("grp", "ep"), None, None, None),
        P(("grp", "ep"), None, None, None),
        P(("grp", "ep"), None, None),
        P(("grp", "ep")),
        P("grp", "ep"),
        P(None, "ep"),
        P(),
        P("ep", None, None),
        P("ep", None, None),
        P("ep", None, None),
        P("ep", None),
        P("ep", None),
        P(None, "ep"),
        P("grp", None),
        P("grp", None),
    )
    return jax.shard_map(
        on_device, mesh=mesh, in_specs=placed, out_specs=P("grp", "ep"), check_vma=False
    )
```

```python
import functools

import jax
import jax.numpy as jnp
from jax import lax
from jax.experimental import pallas as pl
from jax.experimental.pallas import tpu as pltpu
from jax.sharding import PartitionSpec as P

norm_eps = 1e-06
routed_scale = 2.5
contract_last = (((1,), (1,)), ((), ()))
LANES = 128
VMEM_LIMIT = 67043328
f32 = jnp.float32
bf16 = jnp.bfloat16


def dot_t(a, b):
    return lax.dot_general(a, b, contract_last, preferred_element_type=f32)


def join_lanes(blocks, width):
    if width % LANES == 0:
        return jnp.concatenate([b.astype(bf16) for b in blocks], axis=1)
    rows = blocks[0].shape[0]
    total = len(blocks) * width
    lane = lax.broadcasted_iota(jnp.int32, (rows, LANES), 1)
    pieces = [jnp.zeros((rows, LANES), f32) for _ in range(-(-total // LANES))]
    for k, block in enumerate(blocks):
        at, shift = divmod(k * width, LANES)
        moved = jnp.where(lane < width, block.astype(f32), 0.0)
        if shift:
            moved = pltpu.roll(moved, shift, 1)
        if shift + width <= LANES:
            pieces[at] = pieces[at] + moved
        else:
            pieces[at] = pieces[at] + jnp.where(lane >= shift, moved, 0.0)
            pieces[at + 1] = pieces[at + 1] + jnp.where(lane < shift, moved, 0.0)
    return jnp.concatenate([p.astype(bf16) for p in pieces], axis=1)[:, :total]


def widen(block):
    rows, width = block.shape
    short = -width % LANES
    if not short:
        return block
    return jnp.concatenate([block, jnp.zeros((rows, short), block.dtype)], axis=1)


def layer(
    n,
    lengths_ref,
    q_hbm,
    fresh_hbm,
    vnew_hbm,
    forget_hbm,
    residual_hbm,
    gain_hbm,
    routes_hbm,
    route_scores_hbm,
    keys_hbm,
    values_hbm,
    cumlog_hbm,
    out_w_hbm,
    gate_hbm,
    up_hbm,
    down_hbm,
    sgate_hbm,
    sup_hbm,
    sdown_hbm,
    out_ref,
    q_ref,
    fresh_ref,
    vnew_ref,
    forget_ref,
    residual_ref,
    gain_ref,
    routes_ref,
    route_scores_ref,
    keys,
    values,
    cumlog,
    out_w,
    gate_w,
    up_w,
    down_w,
    sgate_w,
    sup_w,
    sdown_w,
    scores,
    att_buf,
    att_wide,
    stream_buf,
    mid_buf,
    eo_src,
    eo_buf,
    small_sem,
    load_sem,
    key_sem,
    value_sem,
    send_sem,
    recv_sem,
):
    me = lax.axis_index("ep")
    heads, head_size = q_ref.shape[1:]
    key_heads, span = keys.shape[:2]
    groups = heads // key_heads
    rows, width = residual_ref.shape
    model = gate_w.shape[1]
    shared_width = sgate_w.shape[0]
    chunks = key_sem.shape[0]
    chunk = span // chunks

    def key_copy(c):
        part = pl.ds(c * chunk, chunk)
        return pltpu.make_async_copy(keys_hbm.at[0, :, part], keys.at[:, part], key_sem.at[c])

    def value_copy(c):
        part = pl.ds(c * chunk, chunk)
        return pltpu.make_async_copy(values_hbm.at[0, :, part], values.at[:, part], value_sem.at[c])

    cumlog_copy = pltpu.make_async_copy(cumlog_hbm.at[0], cumlog, load_sem.at[0])
    out_w_copy = pltpu.make_async_copy(out_w_hbm, out_w, load_sem.at[1])
    sgate_copy = pltpu.make_async_copy(sgate_hbm, sgate_w, load_sem.at[2])
    sup_copy = pltpu.make_async_copy(sup_hbm, sup_w, load_sem.at[3])
    gate_copy = pltpu.make_async_copy(gate_hbm.at[0], gate_w, load_sem.at[4])
    up_copy = pltpu.make_async_copy(up_hbm.at[0], up_w, load_sem.at[5])
    down_copy = pltpu.make_async_copy(down_hbm.at[0], down_w, load_sem.at[6])
    sdown_copy = pltpu.make_async_copy(sdown_hbm, sdown_w, load_sem.at[7])

    smalls = [
        pltpu.make_async_copy(src, dst, small_sem.at[i])
        for i, (src, dst) in enumerate(
            (
                (q_hbm, q_ref),
                (fresh_hbm, fresh_ref),
                (vnew_hbm, vnew_ref),
                (forget_hbm, forget_ref),
                (routes_hbm, routes_ref),
                (route_scores_hbm, route_scores_ref),
                (residual_hbm, residual_ref),
                (gain_hbm, gain_ref),
            )
        )
    ]
    for copy in smalls[:4]:
        copy.start()
    cumlog_copy.start()
    for c in range(chunks):
        key_copy(c).start()
    for c in range(chunks):
        value_copy(c).start()
    for copy in smalls[4:]:
        copy.start()
    out_w_copy.start()

    barrier = pltpu.get_barrier_semaphore()

    def greet(i, carry):
        pl.semaphore_signal(barrier, inc=1, device_id={"ep": lax.rem(me + i, n)})
        return carry

    lax.fori_loop(1, n, greet, 0)

    def remote(phase, src, dst, peer, slot):
        return pltpu.make_async_remote_copy(
            src_ref=src,
            dst_ref=dst,
            send_sem=send_sem.at[phase, peer],
            recv_sem=recv_sem.at[phase, slot],
            device_id={"ep": peer},
        )

    def spread(phase, buf):
        def one(i, carry):
            peer = lax.rem(me + i, n)
            remote(phase, buf.at[me], buf.at[me], peer, me).start()
            return carry

        lax.fori_loop(1, n, one, 0)

    def arrive(phase, buf):
        def one(i, carry):
            peer = lax.rem(me + i, n)
            remote(phase, buf.at[peer], buf.at[peer], peer, peer).wait_recv()
            return carry

        lax.fori_loop(1, n, one, 0)

    def sent(phase, buf):
        def one(i, carry):
            peer = lax.rem(me + i, n)
            remote(phase, buf.at[peer], buf.at[peer], peer, peer).wait_send()
            return carry

        lax.fori_loop(1, n, one, 0)

    for copy in smalls[:4]:
        copy.wait()
    inv_root = head_size ** (-0.5)
    length = lengths_ref[0]
    q = q_ref[0]
    head_row = lax.broadcasted_iota(jnp.int32, (heads, head_size), 0)
    q_wide = jnp.concatenate(
        [jnp.where(head_row // groups == k, q, jnp.zeros_like(q)) for k in range(key_heads)], axis=1
    )
    fresh, vnew = fresh_ref[0].astype(f32), vnew_ref[0].astype(f32)
    own_key, own_value = fresh[0:1], vnew[0:1]
    for k in range(1, key_heads):
        own_key = jnp.where(head_row // groups == k, fresh[k : k + 1], own_key)
        own_value = jnp.where(head_row // groups == k, vnew[k : k + 1], own_value)
    own_score = jnp.sum(q.astype(f32) * own_key, axis=1, keepdims=True) * inv_root
    eye = lax.broadcasted_iota(jnp.int32, (heads, heads), 0) == lax.broadcasted_iota(
        jnp.int32, (heads, heads), 1
    )
    forget = jnp.sum(jnp.where(eye, forget_ref[...], 0.0), axis=1, keepdims=True)
    log_gate = jnp.minimum(forget, 0.0) - jnp.log1p(jnp.exp(-jnp.abs(forget)))

    cumlog_copy.wait()
    position = lax.broadcasted_iota(jnp.int32, (heads, span), 1)
    latest = (
        jnp.sum(jnp.where(position == length - 1, cumlog[...], 0.0), axis=1, keepdims=True)
        + log_gate
    )
    place = lax.broadcasted_iota(jnp.int32, (heads, chunk), 1)
    top = own_score
    for c in range(chunks):
        key_copy(c).wait()
        part = slice(c * chunk, (c + 1) * chunk)
        both = jnp.concatenate([keys[k, part] for k in range(key_heads)], axis=1)
        score = dot_t(q_wide, both) * inv_root + latest - cumlog[:, part]
        score = jnp.where(place + c * chunk < length, score, -jnp.inf)
        scores[:, part] = score
        top = jnp.maximum(top, jnp.max(score, axis=1, keepdims=True))

    sgate_copy.start()
    sup_copy.start()
    gate_copy.start()
    up_copy.start()
    down_copy.start()
    sdown_copy.start()

    own_weight = jnp.exp(own_score - top)
    denominator = own_weight
    weighted = jnp.zeros((heads, key_heads * head_size), f32)
    for c in range(chunks):
        value_copy(c).wait()
        part = slice(c * chunk, (c + 1) * chunk)
        weight = jnp.exp(scores[:, part] - top)
        denominator = denominator + jnp.sum(weight, axis=1, keepdims=True)
        both = jnp.concatenate([values[k, part] for k in range(key_heads)], axis=1)
        weighted = weighted + jnp.dot(weight.astype(bf16), both, preferred_element_type=f32)
    mine = weighted[:, :head_size]
    for k in range(1, key_heads):
        mine = jnp.where(
            head_row // groups == k, weighted[:, k * head_size : (k + 1) * head_size], mine
        )
    numerator = mine + own_weight.astype(bf16).astype(f32) * own_value
    att_buf[me] = (numerator / denominator).astype(bf16)

    pl.semaphore_wait(barrier, n - 1)
    spread(0, att_buf)

    for copy in smalls[4:]:
        copy.wait()
    route_scores = route_scores_ref[...]
    gate_weights = (
        route_scores / jnp.sum(route_scores, axis=0, keepdims=True) * routed_scale
    )
    expert_row = lax.broadcasted_iota(jnp.int32, (n, rows), 0)
    share = jnp.zeros((n, rows), f32)
    for k in range(routes_ref.shape[0]):
        share = share + jnp.where(
            routes_ref[k : k + 1] == expert_row, gate_weights[k : k + 1], 0.0
        )
    row_eye = lax.broadcasted_iota(jnp.int32, (rows, rows), 0) == lax.broadcasted_iota(
        jnp.int32, (rows, rows), 1
    )
    shares = [
        jnp.sum(jnp.where(row_eye, share[e : e + 1], 0.0), axis=1, keepdims=True)
        for e in range(n)
    ]
    out_w_copy.wait()

    arrive(0, att_buf)
    att_wide[...] = att_buf[...].astype(f32).reshape(n * heads, head_size)
    attended = jnp.concatenate(
        [att_wide[pl.ds(h, n, stride=heads), :].astype(bf16) for h in range(heads)], axis=1
    )
    mixed = jnp.dot(attended, out_w[...], preferred_element_type=f32)
    stream = (residual_ref[...].astype(f32) + mixed).astype(bf16)
    stream_buf[me] = widen(stream)
    spread(1, stream_buf)
    sgate_copy.wait()
    sup_copy.wait()
    gate_copy.wait()
    up_copy.wait()
    arrive(1, stream_buf)

    full = join_lanes([stream_buf[j] for j in range(n)], width).astype(f32)
    inv_rms = lax.rsqrt(jnp.mean(full * full, axis=1, keepdims=True) + norm_eps)
    normed = (full * inv_rms * gain_ref[...]).astype(bf16)

    def hidden_of(gate, up):
        gated = dot_t(normed, gate)
        return (jax.nn.silu(gated) * dot_t(normed, up)).astype(bf16)

    mid_buf[me] = widen(hidden_of(sgate_w[...], sup_w[...]))
    spread(2, mid_buf)

    hidden = hidden_of(gate_w[...], up_w[...])
    down_copy.wait()
    wide = max(width, 2 * LANES)
    per = wide // width
    turns = model // wide

    def send_block(peer):
        remote(3, eo_src.at[peer], eo_buf.at[me], peer, me).start()

    for i in range(turns):
        c = lax.rem(me // per + 1 + i, turns)
        part = pl.ds(pl.multiple_of(c * wide, wide), wide)
        out = jnp.dot(hidden, down_w[:, part], preferred_element_type=f32).astype(bf16)
        for s in range(per):
            peer = c * per + s
            eo_src[peer] = widen(out[:, s * width : (s + 1) * width])
        for s in range(per):
            peer = c * per + s
            if i < turns - 1:
                send_block(peer)
            else:
                pl.when(peer != me)(functools.partial(send_block, peer))
    eo_buf[me] = eo_src[me]

    sdown_copy.wait()
    arrive(2, mid_buf)
    mid = join_lanes([mid_buf[j] for j in range(n)], shared_width)
    total = stream.astype(f32) + jnp.dot(mid, sdown_w[...], preferred_element_type=f32)
    arrive(3, eo_buf)
    for e in range(n):
        total = total + shares[e] * eo_buf[e][:, :width].astype(f32)
    out_ref[...] = total.astype(bf16)

    sent(0, att_buf)
    sent(1, stream_buf)
    sent(2, mid_buf)
    sent(3, eo_buf)


def solution(mesh):
    n = mesh.shape["ep"]

    def on_device(
        queries,
        fresh_token_key,
        value_new,
        forget_logit,
        cache_keys,
        cache_values,
        cache_cumlog,
        lengths,
        residual,
        out_weight,
        norm_gain,
        expert_gate,
        expert_up,
        expert_down,
        shared_gate,
        shared_up,
        shared_down,
        routes,
        route_scores,
    ):
        rows, width = residual.shape
        heads, head_size = queries.shape[1:]
        span = cache_keys.shape[2]
        lanes = -(-width // LANES) * LANES
        mid_lanes = -(-shared_gate.shape[0] // LANES) * LANES
        chunks = 4
        vmem = pl.BlockSpec(memory_space=pltpu.VMEM)
        hbm = pl.BlockSpec(memory_space=pltpu.HBM)

        def like(a, drop=0):
            return pltpu.VMEM(a.shape[drop:], a.dtype)

        return pl.pallas_call(
            functools.partial(layer, n),
            out_shape=jax.ShapeDtypeStruct((rows, width), bf16),
            in_specs=[pl.BlockSpec(memory_space=pltpu.SMEM)] + [hbm] * 18,
            out_specs=vmem,
            scratch_shapes=[
                like(queries),
                like(fresh_token_key),
                like(value_new),
                like(forget_logit),
                like(residual),
                pltpu.VMEM((1, norm_gain.shape[0]), f32),
                pltpu.VMEM(routes.shape[::-1], routes.dtype),
                pltpu.VMEM(route_scores.shape[::-1], f32),
                like(cache_keys, 1),
                like(cache_values, 1),
                like(cache_cumlog, 1),
                like(out_weight),
                like(expert_gate, 1),
                like(expert_up, 1),
                like(expert_down, 1),
                like(shared_gate),
                like(shared_up),
                like(shared_down),
                pltpu.VMEM((heads, span), f32),
                pltpu.VMEM((n, heads, head_size), bf16),
                pltpu.VMEM((n * heads, head_size), f32),
                pltpu.VMEM((n, rows, lanes), bf16),
                pltpu.VMEM((n, rows, mid_lanes), bf16),
                pltpu.VMEM((n, rows, lanes), bf16),
                pltpu.VMEM((n, rows, lanes), bf16),
                pltpu.SemaphoreType.DMA((8,)),
                pltpu.SemaphoreType.DMA((8,)),
                pltpu.SemaphoreType.DMA((chunks,)),
                pltpu.SemaphoreType.DMA((chunks,)),
                pltpu.SemaphoreType.DMA((4, n)),
                pltpu.SemaphoreType.DMA((4, n)),
            ],
            compiler_params=pltpu.CompilerParams(
                collective_id=0, has_side_effects=True, vmem_limit_bytes=VMEM_LIMIT
            ),
            name="layer",
        )(
            lengths,
            queries,
            fresh_token_key,
            value_new,
            forget_logit,
            residual,
            norm_gain.reshape(1, -1),
            routes.T,
            route_scores.T,
            cache_keys,
            cache_values,
            cache_cumlog,
            out_weight,
            expert_gate,
            expert_up,
            expert_down,
            shared_gate,
            shared_up,
            shared_down,
        )

    placed = (
        P(("grp", "ep"), None, None),
        P(("grp", "ep"), None, None),
        P(("grp", "ep"), None, None),
        P(("grp", "ep"), None),
        P(("grp", "ep"), None, None, None),
        P(("grp", "ep"), None, None, None),
        P(("grp", "ep"), None, None),
        P(("grp", "ep")),
        P("grp", "ep"),
        P(None, "ep"),
        P(),
        P("ep", None, None),
        P("ep", None, None),
        P("ep", None, None),
        P("ep", None),
        P("ep", None),
        P(None, "ep"),
        P("grp", None),
        P("grp", None),
    )
    return jax.shard_map(
        on_device, mesh=mesh, in_specs=placed, out_specs=P("grp", "ep"), check_vma=False
    )
```

```python
import functools

import jax
import jax.numpy as jnp
from jax import lax
from jax.experimental import pallas as pl
from jax.experimental.pallas import tpu as pltpu
from jax.sharding import PartitionSpec as P

norm_eps = 1e-06
routed_scale = 2.5
contract_last = (((1,), (1,)), ((), ()))
LANES = 128
VMEM_LIMIT = 67043328
f32 = jnp.float32
bf16 = jnp.bfloat16


def dot_t(a, b):
    return lax.dot_general(a, b, contract_last, preferred_element_type=f32)


def join_lanes(blocks, width):
    if width % LANES == 0:
        return jnp.concatenate([b.astype(bf16) for b in blocks], axis=1)
    rows = blocks[0].shape[0]
    total = len(blocks) * width
    lane = lax.broadcasted_iota(jnp.int32, (rows, LANES), 1)
    pieces = [jnp.zeros((rows, LANES), f32) for _ in range(-(-total // LANES))]
    for k, block in enumerate(blocks):
        at, shift = divmod(k * width, LANES)
        moved = jnp.where(lane < width, block.astype(f32), 0.0)
        if shift:
            moved = pltpu.roll(moved, shift, 1)
        if shift + width <= LANES:
            pieces[at] = pieces[at] + moved
        else:
            pieces[at] = pieces[at] + jnp.where(lane >= shift, moved, 0.0)
            pieces[at + 1] = pieces[at + 1] + jnp.where(lane < shift, moved, 0.0)
    return jnp.concatenate([p.astype(bf16) for p in pieces], axis=1)[:, :total]


def widen(block):
    rows, width = block.shape
    short = -width % LANES
    if not short:
        return block
    return jnp.concatenate([block, jnp.zeros((rows, short), block.dtype)], axis=1)


def layer(
    n,
    lengths_ref,
    q_hbm,
    fresh_hbm,
    vnew_hbm,
    forget_hbm,
    residual_hbm,
    gain_hbm,
    routes_hbm,
    route_scores_hbm,
    keys_hbm,
    values_hbm,
    cumlog_hbm,
    out_w_hbm,
    gate_hbm,
    up_hbm,
    down_hbm,
    sgate_hbm,
    sup_hbm,
    sdown_hbm,
    out_ref,
    q_ref,
    fresh_ref,
    vnew_ref,
    forget_ref,
    residual_ref,
    gain_ref,
    routes_ref,
    route_scores_ref,
    keys,
    values,
    cumlog,
    out_w,
    gate_w,
    up_w,
    down_w,
    sgate_w,
    sup_w,
    sdown_w,
    scores,
    att_buf,
    att_wide,
    stream_buf,
    mid_buf,
    eo_src,
    eo_buf,
    small_sem,
    load_sem,
    key_sem,
    value_sem,
    send_sem,
    recv_sem,
):
    me = lax.axis_index("ep")
    heads, head_size = q_ref.shape[1:]
    key_heads, span = keys.shape[:2]
    groups = heads // key_heads
    rows, width = residual_ref.shape
    model = gate_w.shape[1]
    shared_width = sgate_w.shape[0]
    chunks = key_sem.shape[0]
    chunk = span // chunks

    def key_copy(c):
        part = pl.ds(c * chunk, chunk)
        return pltpu.make_async_copy(keys_hbm.at[0, :, part], keys.at[:, part], key_sem.at[c])

    def value_copy(c):
        part = pl.ds(c * chunk, chunk)
        return pltpu.make_async_copy(values_hbm.at[0, :, part], values.at[:, part], value_sem.at[c])

    cumlog_copy = pltpu.make_async_copy(cumlog_hbm.at[0], cumlog, load_sem.at[0])
    out_w_copy = pltpu.make_async_copy(out_w_hbm, out_w, load_sem.at[1])
    sgate_copy = pltpu.make_async_copy(sgate_hbm, sgate_w, load_sem.at[2])
    sup_copy = pltpu.make_async_copy(sup_hbm, sup_w, load_sem.at[3])
    gate_copy = pltpu.make_async_copy(gate_hbm.at[0], gate_w, load_sem.at[4])
    up_copy = pltpu.make_async_copy(up_hbm.at[0], up_w, load_sem.at[5])
    down_copy = pltpu.make_async_copy(down_hbm.at[0], down_w, load_sem.at[6])
    sdown_copy = pltpu.make_async_copy(sdown_hbm, sdown_w, load_sem.at[7])

    smalls = [
        pltpu.make_async_copy(src, dst, small_sem.at[i])
        for i, (src, dst) in enumerate(
            (
                (q_hbm, q_ref),
                (fresh_hbm, fresh_ref),
                (vnew_hbm, vnew_ref),
                (forget_hbm, forget_ref),
                (routes_hbm, routes_ref),
                (route_scores_hbm, route_scores_ref),
                (residual_hbm, residual_ref),
                (gain_hbm, gain_ref),
            )
        )
    ]
    for copy in smalls[:4]:
        copy.start()
    cumlog_copy.start()
    for c in range(chunks):
        key_copy(c).start()
    for c in range(chunks):
        value_copy(c).start()
    for copy in smalls[4:]:
        copy.start()
    out_w_copy.start()

    barrier = pltpu.get_barrier_semaphore()

    def greet(i, carry):
        pl.semaphore_signal(barrier, inc=1, device_id={"ep": lax.rem(me + i, n)})
        return carry

    lax.fori_loop(1, n, greet, 0)

    def remote(phase, src, dst, peer, slot):
        return pltpu.make_async_remote_copy(
            src_ref=src,
            dst_ref=dst,
            send_sem=send_sem.at[phase, peer],
            recv_sem=recv_sem.at[phase, slot],
            device_id={"ep": peer},
        )

    wide = max(width, 2 * LANES)
    per = wide // width
    turns = model // wide
    home = me // per
    toward = 1 - 2 * (home // (turns // 2))

    def visit(i):
        return lax.rem(home + toward * i + turns, turns)

    def spread(phase, buf):
        def one(i, carry):
            peer = lax.rem(me + toward * (n - i) + n, n)
            remote(phase, buf.at[me], buf.at[me], peer, me).start()
            return carry

        lax.fori_loop(1, n, one, 0)

    def arrive(phase, buf):
        def one(i, carry):
            peer = lax.rem(me + i, n)
            remote(phase, buf.at[peer], buf.at[peer], peer, peer).wait_recv()
            return carry

        lax.fori_loop(1, n, one, 0)

    def sent(phase, buf):
        def one(i, carry):
            peer = lax.rem(me + i, n)
            remote(phase, buf.at[peer], buf.at[peer], peer, peer).wait_send()
            return carry

        lax.fori_loop(1, n, one, 0)

    for copy in smalls[:4]:
        copy.wait()
    inv_root = head_size ** (-0.5)
    length = lengths_ref[0]
    q = q_ref[0]
    head_row = lax.broadcasted_iota(jnp.int32, (heads, head_size), 0)
    q_wide = jnp.concatenate(
        [jnp.where(head_row // groups == k, q, jnp.zeros_like(q)) for k in range(key_heads)], axis=1
    )
    fresh, vnew = fresh_ref[0].astype(f32), vnew_ref[0].astype(f32)
    own_key, own_value = fresh[0:1], vnew[0:1]
    for k in range(1, key_heads):
        own_key = jnp.where(head_row // groups == k, fresh[k : k + 1], own_key)
        own_value = jnp.where(head_row // groups == k, vnew[k : k + 1], own_value)
    own_score = jnp.sum(q.astype(f32) * own_key, axis=1, keepdims=True) * inv_root
    eye = lax.broadcasted_iota(jnp.int32, (heads, heads), 0) == lax.broadcasted_iota(
        jnp.int32, (heads, heads), 1
    )
    forget = jnp.sum(jnp.where(eye, forget_ref[...], 0.0), axis=1, keepdims=True)
    log_gate = jnp.minimum(forget, 0.0) - jnp.log1p(jnp.exp(-jnp.abs(forget)))

    cumlog_copy.wait()
    position = lax.broadcasted_iota(jnp.int32, (heads, span), 1)
    latest = (
        jnp.sum(jnp.where(position == length - 1, cumlog[...], 0.0), axis=1, keepdims=True)
        + log_gate
    )
    place = lax.broadcasted_iota(jnp.int32, (heads, chunk), 1)
    top = own_score
    for c in range(chunks):
        key_copy(c).wait()
        part = slice(c * chunk, (c + 1) * chunk)
        both = jnp.concatenate([keys[k, part] for k in range(key_heads)], axis=1)
        score = dot_t(q_wide, both) * inv_root + latest - cumlog[:, part]
        score = jnp.where(place + c * chunk < length, score, -jnp.inf)
        scores[:, part] = score
        top = jnp.maximum(top, jnp.max(score, axis=1, keepdims=True))

    sgate_copy.start()
    sup_copy.start()
    gate_copy.start()
    up_copy.start()
    down_copy.start()
    sdown_copy.start()

    own_weight = jnp.exp(own_score - top)
    denominator = own_weight
    weighted = jnp.zeros((heads, key_heads * head_size), f32)
    for c in range(chunks):
        value_copy(c).wait()
        part = slice(c * chunk, (c + 1) * chunk)
        weight = jnp.exp(scores[:, part] - top)
        denominator = denominator + jnp.sum(weight, axis=1, keepdims=True)
        both = jnp.concatenate([values[k, part] for k in range(key_heads)], axis=1)
        weighted = weighted + jnp.dot(weight.astype(bf16), both, preferred_element_type=f32)
    mine = weighted[:, :head_size]
    for k in range(1, key_heads):
        mine = jnp.where(
            head_row // groups == k, weighted[:, k * head_size : (k + 1) * head_size], mine
        )
    numerator = mine + own_weight.astype(bf16).astype(f32) * own_value
    att_buf[me] = (numerator / denominator).astype(bf16)

    pl.semaphore_wait(barrier, n - 1)
    spread(0, att_buf)

    for copy in smalls[4:]:
        copy.wait()
    route_scores = route_scores_ref[...]
    gate_weights = (
        route_scores / jnp.sum(route_scores, axis=0, keepdims=True) * routed_scale
    )
    expert_row = lax.broadcasted_iota(jnp.int32, (n, rows), 0)
    share = jnp.zeros((n, rows), f32)
    for k in range(routes_ref.shape[0]):
        share = share + jnp.where(
            routes_ref[k : k + 1] == expert_row, gate_weights[k : k + 1], 0.0
        )
    row_eye = lax.broadcasted_iota(jnp.int32, (rows, rows), 0) == lax.broadcasted_iota(
        jnp.int32, (rows, rows), 1
    )
    shares = [
        jnp.sum(jnp.where(row_eye, share[e : e + 1], 0.0), axis=1, keepdims=True)
        for e in range(n)
    ]
    out_w_copy.wait()

    arrive(0, att_buf)
    att_wide[...] = att_buf[...].astype(f32).reshape(n * heads, head_size)
    attended = jnp.concatenate(
        [att_wide[pl.ds(h, n, stride=heads), :].astype(bf16) for h in range(heads)], axis=1
    )
    mixed = jnp.dot(attended, out_w[...], preferred_element_type=f32)
    stream = (residual_ref[...].astype(f32) + mixed).astype(bf16)
    stream_buf[me] = widen(stream)
    spread(1, stream_buf)
    sgate_copy.wait()
    sup_copy.wait()
    gate_copy.wait()
    up_copy.wait()

    def here(peer):
        remote(1, stream_buf.at[peer], stream_buf.at[peer], peer, peer).wait_recv()

    weights = (sgate_w, sup_w, gate_w, up_w)
    sums = [jnp.zeros((rows, w.shape[0]), f32) for w in weights]
    squares = jnp.zeros((rows, 1), f32)
    for i in range(turns):
        c = visit(i)
        part = pl.ds(pl.multiple_of(c * wide, wide), wide)
        for t in range(per):
            peer = c * per + t
            if i:
                here(peer)
            else:
                pl.when(peer != me)(functools.partial(here, peer))
        block = join_lanes([stream_buf[c * per + t] for t in range(per)], width).astype(f32)
        squares = squares + jnp.sum(block * block, axis=1, keepdims=True)
        scaled = (block * gain_ref[:, part]).astype(bf16)
        sums = [total + dot_t(scaled, w[:, part]) for total, w in zip(sums, weights)]
    inv_rms = lax.rsqrt(squares * (1.0 / model) + norm_eps)
    sgated, supped, gated, upped = [total * inv_rms for total in sums]

    mid_buf[me] = widen((jax.nn.silu(sgated) * supped).astype(bf16))
    spread(2, mid_buf)

    hidden = (jax.nn.silu(gated) * upped).astype(bf16)
    down_copy.wait()

    def send_block(peer):
        remote(3, eo_src.at[peer], eo_buf.at[me], peer, me).start()

    for i in range(turns):
        c = visit(turns - 1 - i)
        part = pl.ds(pl.multiple_of(c * wide, wide), wide)
        out = jnp.dot(hidden, down_w[:, part], preferred_element_type=f32).astype(bf16)
        for s in range(per):
            peer = c * per + s
            eo_src[peer] = widen(out[:, s * width : (s + 1) * width])
        for s in range(per):
            peer = c * per + s
            if i < turns - 1:
                send_block(peer)
            else:
                pl.when(peer != me)(functools.partial(send_block, peer))
    eo_buf[me] = eo_src[me]

    sdown_copy.wait()
    arrive(2, mid_buf)
    mid = join_lanes([mid_buf[j] for j in range(n)], shared_width)
    total = stream.astype(f32) + jnp.dot(mid, sdown_w[...], preferred_element_type=f32)
    arrive(3, eo_buf)
    for e in range(n):
        total = total + shares[e] * eo_buf[e][:, :width].astype(f32)
    out_ref[...] = total.astype(bf16)

    sent(0, att_buf)
    sent(1, stream_buf)
    sent(2, mid_buf)
    sent(3, eo_buf)


def solution(mesh):
    n = mesh.shape["ep"]

    def on_device(
        queries,
        fresh_token_key,
        value_new,
        forget_logit,
        cache_keys,
        cache_values,
        cache_cumlog,
        lengths,
        residual,
        out_weight,
        norm_gain,
        expert_gate,
        expert_up,
        expert_down,
        shared_gate,
        shared_up,
        shared_down,
        routes,
        route_scores,
    ):
        rows, width = residual.shape
        heads, head_size = queries.shape[1:]
        span = cache_keys.shape[2]
        lanes = -(-width // LANES) * LANES
        mid_lanes = -(-shared_gate.shape[0] // LANES) * LANES
        chunks = 4
        vmem = pl.BlockSpec(memory_space=pltpu.VMEM)
        hbm = pl.BlockSpec(memory_space=pltpu.HBM)

        def like(a, drop=0):
            return pltpu.VMEM(a.shape[drop:], a.dtype)

        return pl.pallas_call(
            functools.partial(layer, n),
            out_shape=jax.ShapeDtypeStruct((rows, width), bf16),
            in_specs=[pl.BlockSpec(memory_space=pltpu.SMEM)] + [hbm] * 18,
            out_specs=vmem,
            scratch_shapes=[
                like(queries),
                like(fresh_token_key),
                like(value_new),
                like(forget_logit),
                like(residual),
                pltpu.VMEM((1, norm_gain.shape[0]), f32),
                pltpu.VMEM(routes.shape[::-1], routes.dtype),
                pltpu.VMEM(route_scores.shape[::-1], f32),
                like(cache_keys, 1),
                like(cache_values, 1),
                like(cache_cumlog, 1),
                like(out_weight),
                like(expert_gate, 1),
                like(expert_up, 1),
                like(expert_down, 1),
                like(shared_gate),
                like(shared_up),
                like(shared_down),
                pltpu.VMEM((heads, span), f32),
                pltpu.VMEM((n, heads, head_size), bf16),
                pltpu.VMEM((n * heads, head_size), f32),
                pltpu.VMEM((n, rows, lanes), bf16),
                pltpu.VMEM((n, rows, mid_lanes), bf16),
                pltpu.VMEM((n, rows, lanes), bf16),
                pltpu.VMEM((n, rows, lanes), bf16),
                pltpu.SemaphoreType.DMA((8,)),
                pltpu.SemaphoreType.DMA((8,)),
                pltpu.SemaphoreType.DMA((chunks,)),
                pltpu.SemaphoreType.DMA((chunks,)),
                pltpu.SemaphoreType.DMA((4, n)),
                pltpu.SemaphoreType.DMA((4, n)),
            ],
            compiler_params=pltpu.CompilerParams(
                collective_id=0, has_side_effects=True, vmem_limit_bytes=VMEM_LIMIT
            ),
            name="layer",
        )(
            lengths,
            queries,
            fresh_token_key,
            value_new,
            forget_logit,
            residual,
            norm_gain.reshape(1, -1),
            routes.T,
            route_scores.T,
            cache_keys,
            cache_values,
            cache_cumlog,
            out_weight,
            expert_gate,
            expert_up,
            expert_down,
            shared_gate,
            shared_up,
            shared_down,
        )

    placed = (
        P(("grp", "ep"), None, None),
        P(("grp", "ep"), None, None),
        P(("grp", "ep"), None, None),
        P(("grp", "ep"), None),
        P(("grp", "ep"), None, None, None),
        P(("grp", "ep"), None, None, None),
        P(("grp", "ep"), None, None),
        P(("grp", "ep")),
        P("grp", "ep"),
        P(None, "ep"),
        P(),
        P("ep", None, None),
        P("ep", None, None),
        P("ep", None, None),
        P("ep", None),
        P("ep", None),
        P(None, "ep"),
        P("grp", None),
        P("grp", None),
    )
    return jax.shard_map(
        on_device, mesh=mesh, in_specs=placed, out_specs=P("grp", "ep"), check_vma=False
    )
```
